32 devices in a mesh: sp: 8 (over z, x), tp: 4 (over y, core).
Axes of the slice: x: 2, y: 2, z: 4, core: 2. Of those that a mesh axis runs over, the one named last changes fastest.
Arguments:
- mixer_in: bfloat16 [2048, 2048], P('sp', 'tp'), may hold values from -6 to 6
- doc_ids: int32 [2048], P('sp'), may hold values from 0 to 3, never falling along the last dimension, each value on 1 to 1024 neighbouring positions
- mix_scale: float32 [2048], P('tp'), may hold values from 0.1 to 1.9
- out_proj: bfloat16 [2048, 2048], P('tp'), may hold values from -0.125 to 0.125
- residual: bfloat16 [2048, 2048], P('sp'), may hold values from -6 to 6
- mix_gain: float32 [2048], replicated, may hold values from 0.1 to 1.9
- expert_ids: int32 [2048, 2], P('sp'), may hold values from 0 to 7, all different within a row; in each aligned block of 256 rows (0 to 255, 256 to 511, ...) at most 128 rows name the same one
- expert_weight: float32 [2048, 2], P('sp'), may hold values from 0.2 to 1
- w_gate: bfloat16 [8, 2048, 5632], P('sp', None, 'tp'), may hold values from -0.125 to 0.125
- w_up: bfloat16 [8, 2048, 5632], P('sp', None, 'tp'), may hold values from -0.125 to 0.125
- w_down: bfloat16 [8, 5632, 2048], P('sp', 'tp'), may hold values from -0.078125 to 0.078125
- out_gain: float32 [2048], replicated, may hold values from 0.1 to 1.9
Outputs:
- layer_out: bfloat16 [2048, 2048], P('sp')
The draws below stay inside these ranges and needn't reach their ends.
Inputs may be any that keep to these rules, and one draw needn't show every extreme that they name: `doc_ids`: document numbers never fall along the tokens; a document has at most 1024 positions. `expert_ids`: A row's two experts differ. In each aligned block of 256 rows (the tokens of one index of sp) no expert is named by more than 128 rows; some block has an expert named by exactly 128 rows.
All inputs are finite; a program needn't handle non-finite values.
Results may differ from the reference program's by a relative error of at most 0.015.
Values may be sent and summed in bfloat16 or wider, within the bound.
No kernel may reach another device: no remote copies, remote signals or barrier semaphores. Data moves between devices by JAX's collectives and lax.ppermute only.
A program may use at most 64 MiB of HBM per device.

```python
import math
import jax
import jax.numpy as jnp
import numpy as np
from jax import lax

D = 2048
FF = 5632
TOK_SP = 256
TOKENS = 2048
EXPERTS = 8
CAP = 128
FF_DEV = 1408
N_SP = 8
N_TP = 4


def block_scale(own_key, dims, pieces, smallest, top_value):
    def one(position, shards_of):
        draws = jax.random.uniform(jax.random.fold_in(jax.random.fold_in(own_key, 6), position), (shards_of,), jnp.float32, smallest / len(pieces), top_value / len(pieces))
        return jnp.repeat(jnp.exp(draws), dims[position] // shards_of).reshape((-1,) + (1,) * (len(dims) - position - 1))

    level = one(*pieces[0])
    for cut in pieces[1:]:
        level = level * one(*cut)
    return level


def profile(amount, total, limit, slope):
    weights = [(1 << 20) // math.isqrt(grade ** slope) + 1 for grade in range(2, amount + 1)]
    surplus, given = total - limit - (amount - 1), [1] * (amount - 1)
    while surplus > 0:
        free = [i for i in range(amount - 1) if given[i] < limit]
        mass, remaining = sum([weights[i] for i in free]), surplus
        for i in free:
            extra = min(limit - given[i], max(1, remaining * weights[i] // mass), surplus)
            given[i] = given[i] + extra
            surplus = surplus - extra
    return np.array([limit] + given)


def uneven_parts(rng, count, total, reach, lean):
    if count == 2:
        one = jax.random.randint(rng, (), max(1, total - reach), min(reach, total - 1) + 1)
        return jnp.stack([one, total - one])
    sizes = jnp.asarray(profile(count, total, reach, lean), jnp.int32)
    pairs = (count - 1) // 2
    donor, sink = sizes[1:1 + 2 * pairs:2], sizes[2:2 + 2 * pairs:2]
    room = jnp.minimum(donor - 1, reach - sink)
    moved = jax.random.randint(jax.random.fold_in(rng, 1), (pairs,), 0, 1 << 20) % (room + 1)
    sizes = sizes.at[1:1 + 2 * pairs:2].set(donor - moved).at[2:2 + 2 * pairs:2].set(sink + moved)
    return sizes[jax.random.permutation(jax.random.fold_in(rng, 2), count)]


def shared_out(key, own, number, rows, number_of, top, limit, slope):
    sequence = jax.random.permutation(key, number_of)
    packed, usual = shares(number_of, rows * top, limit, slope, True), shares(number_of, rows * top, limit, slope, False)
    places = jnp.arange(number_of)

    def named(sizes, offset_by):
        used = int((sizes > 0).sum())
        fixed = max(1, used // 4)
        moved = fixed + (places - fixed + offset_by * (used - fixed)) % max(1, number_of - fixed)
        return jnp.zeros((number_of,), jnp.int32).at[sequence[jnp.where(places < fixed, places, moved)]].set(jnp.asarray(sizes, jnp.int32))

    sizes = jnp.where(number % 4 == 0, named(packed, number // 4), named(usual, number - number // 4 - 1))
    mixed = jax.random.permutation(jax.random.fold_in(own, 3), number_of)
    giver, sink = mixed[0:number_of // 2 * 2:2], mixed[1:number_of // 2 * 2:2]
    margin = jnp.minimum(sizes[giver] - 1, limit - sizes[sink]) // 2
    margin = jnp.where((giver == sequence[0]) | (sink == sequence[0]) | (sizes[sink] == 0), 0, jnp.maximum(margin, 0))
    moved = jax.random.randint(jax.random.fold_in(own, 4), (number_of // 2,), 0, 1 << 20) % (margin + 1)
    sizes = sizes.at[giver].add(-moved).at[sink].add(moved)
    members = jnp.searchsorted(jnp.cumsum(sizes), jnp.arange(rows * top), side="right").astype(jnp.int32)
    table = members.reshape(top, rows).T
    table = table[jax.random.permutation(jax.random.fold_in(own, 1), rows)]
    offset_by = jax.random.randint(jax.random.fold_in(own, 2), (rows, 1), 0, top)
    return jnp.take_along_axis(table, (jnp.arange(top)[None, :] + offset_by) % top, axis=1)


def shares(number_of, total, bound, skew, full):
    portions = [(1 << 20) // math.isqrt(rank ** skew) + 1 for rank in range(1, number_of + 1)]
    largest = bound if full else min(bound, max(-(-total // number_of), total * portions[0] // sum(portions)))
    least = 1 if total - largest >= number_of - 1 else 0
    holding, rest = [largest] + [least] * (number_of - 1), total - largest - least * (number_of - 1)
    while rest > 0:
        movable = [i for i in range(1, number_of) if holding[i] < largest] or [i for i in range(1, number_of) if holding[i] < bound]
        whole, left = sum([portions[i] for i in movable]), rest
        for i in movable:
            extra = min(bound - holding[i], max(1, left * portions[i] // whole), rest)
            holding[i] = holding[i] + extra
            rest = rest - extra
    return np.array(holding)


def scatter_about(stream_key, shape, scale, bound, cuts=(), held_as=jnp.bfloat16):
    factor_of = block_scale(stream_key, shape, cuts, -0.22, 0.18) if cuts else 1.0
    drawn = jax.random.normal(stream_key, shape, jnp.float32) * scale * factor_of
    return jnp.minimum(jnp.maximum(drawn, -bound), bound).astype(held_as)


def setup_inputs(seed: int = 0) -> dict:
    seeds = jax.random.split(jax.random.key(seed), 13)
    mixer_in = scatter_about(seeds[0], (TOKENS, D), 1.0, 6.0, ((0, 8), (1, 4)))
    doc_ids = jnp.searchsorted(jnp.cumsum(uneven_parts(seeds[1], N_SP // 2, TOKENS, 4 * TOK_SP, 1)), jnp.arange(TOKENS), side="right").astype(jnp.int32)
    mix_scale = jnp.clip(1.0 + 0.18 * jax.random.normal(seeds[2], (D,), jnp.float32), 0.1, 1.9)
    out_proj = scatter_about(seeds[3], (D, D), D ** -0.5, 0.125, ((0, 4),))
    residual = scatter_about(seeds[4], (TOKENS, D), 1.0, 6.0, ((0, 8),))
    mix_gain = jnp.clip(1.0 + 0.18 * jax.random.normal(seeds[5], (D,), jnp.float32), 0.1, 1.9)
    expert_ids_keys = jax.random.split(jax.random.fold_in(seeds[6], 1), TOKENS // TOK_SP)
    expert_ids_turns = jax.random.permutation(jax.random.fold_in(seeds[6], 3), TOKENS // TOK_SP)
    expert_ids = jax.vmap(lambda own, number: shared_out(jax.random.fold_in(seeds[6], 2), own, number, TOK_SP, EXPERTS, 2, CAP, 2))(expert_ids_keys, expert_ids_turns).reshape((TOKENS, 2))
    expert_weight = jnp.clip(0.2 + 0.8 * jax.random.uniform(seeds[7], (TOKENS, 2), jnp.float32) ** block_scale(seeds[7], (TOKENS, 2), ((0, 8),), -0.2, 0.2), 0.2, 1.0)
    w_gate = scatter_about(seeds[8], (EXPERTS, D, FF), D ** -0.5, 0.125, ((0, 8), (2, 4)))
    w_up = scatter_about(seeds[9], (EXPERTS, D, FF), D ** -0.5, 0.125, ((0, 8), (2, 4)))
    w_down = scatter_about(seeds[10], (EXPERTS, FF, D), FF ** -0.5, 0.078125, ((0, 8), (1, 4)))
    out_gain = jnp.clip(1.0 + 0.18 * jax.random.normal(seeds[11], (D,), jnp.float32), 0.1, 1.9)
    return dict(mixer_in=mixer_in, doc_ids=doc_ids, mix_scale=mix_scale, out_proj=out_proj, residual=residual, mix_gain=mix_gain, expert_ids=expert_ids, expert_weight=expert_weight, w_gate=w_gate, w_up=w_up, w_down=w_down, out_gain=out_gain)


alpha_res = 1.4142135623730951
norm_eps = 1e-05
pool_reach = 15

def layer_norm(summed, norm_gain):
    row_mean = lax.optimization_barrier(jnp.mean(summed, axis=-1, keepdims=True))
    centred = summed - row_mean
    row_var = lax.optimization_barrier(jnp.mean(centred * centred, axis=-1, keepdims=True))
    return centred * lax.rsqrt(row_var + norm_eps) * norm_gain

def pair_slots(pair_ids, experts):
    flat_ids = pair_ids.reshape(-1)
    onehot = (flat_ids[:, None] == jnp.arange(experts, dtype=jnp.int32)[None, :]).astype(jnp.int32)
    before = jnp.cumsum(onehot, axis=0) - onehot
    return lax.optimization_barrier(jnp.sum(before * onehot, axis=1)).reshape(pair_ids.shape).astype(jnp.int32)

def reference(mixer_in, doc_ids, mix_scale, out_proj, residual, mix_gain, expert_ids, expert_weight, w_gate, w_up, w_down, out_gain):
    tokens, features = mixer_in.shape
    values = mixer_in.astype(jnp.float32)
    positions = jnp.arange(tokens, dtype=jnp.int32)
    channel = jnp.arange(features, dtype=jnp.int32)
    window = jnp.left_shift(jnp.int32(2), (channel // (features // 4)).astype(jnp.int32))
    window_sum = jnp.zeros((tokens, features), jnp.float32)
    window_count = jnp.zeros((tokens, features), jnp.float32)
    for lag_step in range(pool_reach + 1):
        shifted = jnp.concatenate([jnp.zeros((lag_step, features), jnp.float32), values[:tokens - lag_step]], axis=0)
        shifted_doc = jnp.concatenate([jnp.full((lag_step,), -1, jnp.int32), doc_ids[:tokens - lag_step]], axis=0)
        same_doc = (shifted_doc == doc_ids) & (positions >= lag_step)
        in_window = (same_doc[:, None] & (lag_step < window)[None, :]).astype(jnp.float32)
        window_sum = window_sum + in_window * shifted
        window_count = window_count + in_window
    mixed_rows = ((window_sum / window_count - values) * mix_scale).astype(jnp.bfloat16)
    projected = jnp.dot(mixed_rows, out_proj, preferred_element_type=jnp.float32)
    normed = layer_norm(alpha_res * residual.astype(jnp.float32) + projected, mix_gain).astype(jnp.bfloat16)
    experts = w_gate.shape[0]
    blocks = N_SP
    block_rows = tokens // blocks
    capacity = CAP
    ids_blocks = expert_ids.reshape(blocks, block_rows, 2)
    ranks = jax.vmap(lambda pair_ids: pair_slots(pair_ids, experts))(ids_blocks)
    target = (ids_blocks * capacity + ranks).astype(jnp.int32)
    block_index = jnp.broadcast_to(jnp.arange(blocks, dtype=jnp.int32)[:, None, None], target.shape)
    row_index = jnp.broadcast_to(jnp.arange(block_rows, dtype=jnp.int32)[None, :, None], target.shape)
    slot_row = jnp.full((blocks, experts * capacity), block_rows, jnp.int32).at[block_index, target].set(row_index)
    normed_blocks = jnp.concatenate([normed.reshape(blocks, block_rows, features), jnp.zeros((blocks, 1, features), jnp.bfloat16)], axis=1)
    expert_in = jnp.take_along_axis(normed_blocks, slot_row[:, :, None], axis=1)
    expert_in = expert_in.reshape(blocks, experts, capacity, features).transpose(1, 0, 2, 3)

    def one_expert(inputs):
        rows_in, gate_w, up_w, down_w = inputs
        flat_in = rows_in.reshape(-1, features)
        gate_pre = jnp.dot(flat_in, gate_w, preferred_element_type=jnp.float32)
        upper = jnp.dot(flat_in, up_w, preferred_element_type=jnp.float32)
        hidden = (jax.nn.silu(gate_pre) * upper).astype(jnp.bfloat16)
        split_hidden = hidden.reshape(-1, N_TP, FF_DEV).astype(jnp.float32)
        split_down = down_w.reshape(N_TP, FF_DEV, features).astype(jnp.float32)
        parts = jnp.einsum('rjf,jfd->jrd', split_hidden, split_down).astype(jnp.bfloat16)
        return lax.optimization_barrier(jnp.sum(parts.astype(jnp.float32), axis=0)).reshape(blocks, capacity, features)
    outputs = lax.map(one_expert, (expert_in, w_gate, w_up, w_down))
    outputs = outputs.transpose(1, 0, 2, 3).reshape(blocks, experts * capacity, features)
    picked = jnp.take_along_axis(outputs, target.reshape(blocks, -1)[:, :, None], axis=1)
    picked = picked.reshape(blocks, block_rows, 2, features)
    routed = lax.optimization_barrier(jnp.sum(picked * expert_weight.reshape(blocks, block_rows, 2)[..., None], axis=2)).reshape(tokens, features)
    return layer_norm(alpha_res * normed.astype(jnp.float32) + routed, out_gain).astype(jnp.bfloat16)
```

```python
import functools

import jax
import jax.numpy as jnp
from jax import lax
from jax.experimental import pallas as pl
from jax.experimental.pallas import tpu as pltpu
from jax.sharding import PartitionSpec as P

alpha_res = 1.4142135623730951
norm_eps = 1e-05
reach = 16
lanes = 128
f32, bf16 = jnp.float32, jnp.bfloat16
MIB = 2**20


def swap(value, axis, bits):
    if bits == 0:
        return value
    count = lax.axis_size(axis)
    return lax.ppermute(value, axis, [(i, i ^ bits) for i in range(count)])


def tiles(total, width):
    return [(at, min(width, total - at)) for at in range(0, total, width)]


def dot(a, b):
    return jnp.dot(a, b, preferred_element_type=f32)


def call(body, outs, operands, scratch=(), flops=1_000_000, vmem=16, name=None):
    whole = pl.BlockSpec(memory_space=pltpu.VMEM)
    return pl.pallas_call(
        body,
        out_shape=[jax.ShapeDtypeStruct(shape, kind) for shape, kind in outs],
        in_specs=[whole] * len(operands),
        out_specs=[whole] * len(outs),
        scratch_shapes=list(scratch),
        compiler_params=pltpu.CompilerParams(vmem_limit_bytes=vmem * MIB),
        cost_estimate=pl.CostEstimate(flops=flops, bytes_accessed=0, transcendentals=0),
        name=name,
    )(*operands)


def place():
    t = lax.axis_index("tp")
    return t & 1, t >> 1, lax.axis_size("tp") // 2


def columns(start, width):
    return pl.ds(pl.multiple_of(start, lanes), width)


def as_column(row):
    return jnp.broadcast_to(row, (lanes, row.shape[1])).T[:, :1]


def tail_body(x, docs, pack):
    rows = x.shape[0]
    pack[0:reach, :] = x[rows - reach :, :]
    pack[reach:, :] = jnp.zeros_like(pack[reach:, :])
    pack[reach:, 0:lanes] = jnp.broadcast_to(
        docs[:, rows - lanes :].astype(f32), (reach, lanes)
    ).astype(bf16)


def mix_body(x, pack, docs, scale, weights, keep, send):
    core, _, _ = place()
    rows, cols = x.shape
    half = keep.shape[1]
    window = jnp.left_shift(2, lax.axis_index("tp") * cols // (2 * half // 4))
    doc_row = docs[...].astype(f32)
    doc_col = as_column(doc_row)
    lag = lax.broadcasted_iota(jnp.int32, (rows, rows), 0) - lax.broadcasted_iota(
        jnp.int32, (rows, rows), 1
    )
    band = jnp.where((lag >= 0) & (lag < window) & (doc_col == doc_row), 1.0, 0.0)
    total = dot(band.astype(bf16), x[...])
    count = jnp.sum(band, axis=1, keepdims=True)
    lag_tail = (
        lax.broadcasted_iota(jnp.int32, (reach, lanes), 0)
        + lanes
        - lax.broadcasted_iota(jnp.int32, (reach, lanes), 1)
    )
    tail_doc = pack[reach : reach + 1, 0:lanes].astype(f32)
    inside = (lag_tail < window) & (doc_col[:reach] == tail_doc) & (lax.axis_index("sp") > 0)
    band_tail = jnp.where(inside, 1.0, 0.0)
    before = jnp.concatenate(
        [jnp.zeros((lanes - reach, cols), bf16), pack[0:reach, :]], axis=0
    )
    top = total[:reach] + dot(band_tail.astype(bf16), before)
    top_count = count[:reach] + jnp.sum(band_tail, axis=1, keepdims=True)
    total = jnp.concatenate([top, total[reach:]], axis=0)
    count = jnp.concatenate([top_count, count[reach:]], axis=0)
    mixed = ((total / count - x[...].astype(f32)) * scale[...]).astype(bf16)
    for out, which in ((send, 1 - core), (keep, core)):
        for at, width in tiles(half, 256):
            out[:, at : at + width] = dot(
                mixed, weights[:, columns(which * half + at, width)]
            ).astype(out.dtype)


def split_body(keep, arrived, own, *sends):
    _, y, _ = place()
    part = own.shape[1]
    for bits, out in enumerate((own, *sends)):
        at = columns((y ^ bits) * part, part)
        out[...] = (keep[:, at].astype(f32) + arrived[:, at].astype(f32)).astype(out.dtype)


def stats_body(parts, *refs):
    own, arrived, residual, z_out, stats = refs[0], refs[1:parts], refs[parts], refs[-2], refs[-1]
    core, y, y_parts = place()
    width = own.shape[1]
    z = alpha_res * residual[:, columns((core * y_parts + y) * width, width)].astype(f32)
    shares = own[...]
    for ref in arrived:
        shares = shares + ref[...].astype(f32)
    z = z + shares
    z_out[...] = z
    mean = jnp.mean(z, axis=1, keepdims=True)
    spread = jnp.sum((z - mean) * (z - mean), axis=1, keepdims=True)
    lane = lax.broadcasted_iota(jnp.int32, (z.shape[0], lanes), 1)
    stats[...] = jnp.where(lane == 0, mean, spread).T[0:8, :]


def slot_rows(ids, capacity, experts):
    tokens = ids.shape[1]
    expert = lax.broadcasted_iota(jnp.int32, (experts, tokens), 0)
    first, second = expert == ids[0:1, :], expert == ids[1:2, :]
    named = jnp.where(first | second, 1.0, 0.0)
    earlier = (
        lax.broadcasted_iota(jnp.int32, (tokens, tokens), 0)
        < lax.broadcasted_iota(jnp.int32, (tokens, tokens), 1)
    )
    before = dot(named.astype(bf16), jnp.where(earlier, 1.0, 0.0).astype(bf16))
    slots = []
    for k, mine in enumerate((first, second)):
        rank = jnp.sum(jnp.where(mine, before, 0.0), axis=0, keepdims=True)
        slots.append(ids[k : k + 1, :] * capacity + rank.astype(jnp.int32))
    return slots


def dispatch_body(devices, experts, *refs):
    stats, (z_ref, gain, ids), outs = refs[:devices], refs[devices : devices + 3], refs[devices + 3 :]
    normed_ref, sends = outs[0], outs[1:]
    core, y, y_parts = place()
    tokens, width = z_ref.shape
    capacity = sends[0].shape[0]
    means = [ref[0:1, :] for ref in stats]
    mean = sum(means[1:], means[0]) / devices
    spread = sum(
        (ref[1:2, :] + width * (m - mean) * (m - mean) for ref, m in zip(stats, means)),
        jnp.zeros_like(mean),
    )
    scale = lax.rsqrt(spread / (width * devices) + norm_eps)
    gain_here = gain[:, columns((core * y_parts + y) * width, width)]
    normed = (z_ref[...] - as_column(mean)) * as_column(scale) * gain_here
    normed = normed.astype(bf16)
    normed_ref[...] = normed
    slots = slot_rows(ids, capacity, experts)
    s = lax.axis_index("sp")
    for bits, out in enumerate(sends):
        slot = (s ^ bits) * capacity + lax.broadcasted_iota(jnp.int32, (capacity, tokens), 0)
        chosen = jnp.where((slots[0] == slot) | (slots[1] == slot), 1.0, 0.0)
        out[...] = dot(chosen.astype(bf16), normed).astype(bf16)


def stack_body(*refs):
    out = refs[-1]
    rows = refs[0].shape[0]
    for i, ref in enumerate(refs[:-1]):
        out[i * rows : (i + 1) * rows, :] = ref[...]


def unpack(pieces, wide):
    core, y, y_parts = place()
    width = pieces[0].shape[1]
    for i, ref in enumerate(pieces):
        at = (core ^ (i // y_parts)) * y_parts + (y ^ (i % y_parts))
        wide[:, columns(at * width, width)] = ref[...]


def expert_body(count, *refs):
    pieces, (w_gate, w_up, w_down), (send, keep) = (
        refs[:count],
        refs[count : count + 3],
        refs[count + 3 : count + 5],
    )
    wide, hidden = refs[count + 5 :]
    core, _, _ = place()
    unpack(pieces, wide)
    half = keep.shape[1]
    for at, width in tiles(w_gate.shape[1], 256):
        gate = dot(wide[...], w_gate[:, at : at + width])
        upper = dot(wide[...], w_up[:, at : at + width])
        hidden[:, at : at + width] = (gate / (1.0 + jnp.exp(-gate)) * upper).astype(bf16)
    for out, which in ((send, 1 - core), (keep, core)):
        for at, width in tiles(half, 256):
            out[:, at : at + width] = dot(
                hidden[...], w_down[:, columns(which * half + at, width)]
            ).astype(bf16)


def homeward_body(parts, *refs):
    own, arrived, outs = refs[0], refs[1:parts], refs[parts:]
    rows = outs[0].shape[0]
    total = own[...].astype(f32)
    for ref in arrived:
        total = total + ref[...].astype(f32)
    for i, out in enumerate(outs):
        out[...] = total[i * rows : (i + 1) * rows].astype(bf16)


def combine_body(experts, *refs):
    returned, (ids, pair_weight, normed, z_out) = refs[:experts], refs[experts:]
    capacity = returned[0].shape[0]
    tokens = normed.shape[0]
    slots = slot_rows(ids, capacity, experts)
    s = lax.axis_index("sp")
    z = alpha_res * normed[...].astype(f32)
    for bits, ref in enumerate(returned):
        slot = (s ^ bits) * capacity + lax.broadcasted_iota(jnp.int32, (capacity, tokens), 0)
        chosen = jnp.where(slots[0] == slot, pair_weight[0:1, :], 0.0) + jnp.where(
            slots[1] == slot, pair_weight[1:2, :], 0.0
        )
        high = chosen.astype(bf16)
        low = (chosen - high.astype(f32)).astype(bf16)
        for share in (high, low):
            z = z + lax.dot_general(
                share, ref[...], (((0,), (0,)), ((), ())), preferred_element_type=f32
            )
    z_out[...] = z.astype(bf16)


def norm_body(*refs):
    pieces, gain, out, wide = refs[:-3], refs[-3], refs[-2], refs[-1]
    unpack(pieces, wide)
    z = wide[...].astype(f32)
    centred = z - jnp.mean(z, axis=1, keepdims=True)
    var = jnp.mean(centred * centred, axis=1, keepdims=True)
    out[...] = (centred * lax.rsqrt(var + norm_eps) * gain[...]).astype(bf16)


def over_tp(value, y_parts):
    mine = [swap(value, "tp", bits << 1) for bits in range(y_parts)]
    return mine + [swap(part, "tp", 1) for part in mine]


def shards(
    mixer_in,
    doc_ids,
    mix_scale,
    out_proj,
    residual,
    mix_gain,
    expert_ids,
    expert_weight,
    w_gate,
    w_up,
    w_down,
    out_gain,
):
    tokens, cols = mixer_in.shape
    features = mix_gain.shape[0]
    experts, devices = lax.axis_size("sp"), lax.axis_size("tp")
    y_parts = devices // 2
    half, part = features // 2, features // devices
    capacity = 4 * tokens // experts
    docs = doc_ids.reshape(1, tokens)
    ids, pair_weight = expert_ids.T, expert_weight.T

    (pack,) = call(tail_body, [((2 * reach, cols), bf16)], (mixer_in, docs), name="tail")
    pack = lax.ppermute(pack, "sp", [(i, i + 1) for i in range(experts - 1)])
    keep, send = call(
        mix_body,
        [((tokens, half), f32), ((tokens, half), bf16)],
        (mixer_in, pack, docs, mix_scale.reshape(1, cols), out_proj),
        flops=2 * tokens * cols * features,
        name="mix",
    )
    arrived = swap(send, "tp", 1)
    own, *sends = call(
        split_body,
        [((tokens, part), f32)] + [((tokens, part), bf16)] * (y_parts - 1),
        (keep, arrived),
        name="split",
    )
    shares = [swap(v, "tp", (i + 1) << 1) for i, v in enumerate(sends)]
    z, stats = call(
        functools.partial(stats_body, y_parts),
        [((tokens, part), f32), ((8, tokens), f32)],
        (own, *shares, residual),
        name="stats",
    )
    every = [swap(stats, "tp", bits) for bits in range(devices)]
    normed, *outgoing = call(
        functools.partial(dispatch_body, devices, experts),
        [((tokens, part), bf16)] + [((capacity, part), bf16)] * experts,
        (*every, z, mix_gain.reshape(1, features), ids),
        flops=2 * tokens * tokens * part * 4,
        name="dispatch",
    )
    incoming = [swap(v, "sp", bits) for bits, v in enumerate(outgoing)]
    group = experts // 2
    rows = group * capacity
    returned = []
    for first in range(0, experts, group):
        (stacked,) = call(
            stack_body, [((rows, part), bf16)], incoming[first : first + group], name="stack"
        )
        pieces = over_tp(stacked, y_parts)
        send, keep = call(
            functools.partial(expert_body, len(pieces)),
            [((rows, half), bf16)] * 2,
            (*pieces, w_gate[0], w_up[0], w_down[0]),
            scratch=[
                pltpu.VMEM((rows, features), bf16),
                pltpu.VMEM((rows, w_gate.shape[2]), bf16),
            ],
            flops=6 * rows * features * w_gate.shape[2],
            vmem=24,
            name="expert",
        )
        arrived = swap(send, "tp", 1)
        own, *sends = call(
            split_body,
            [((rows, part), bf16)] * y_parts,
            (keep, arrived),
            name="part",
        )
        shares = [swap(v, "tp", (i + 1) << 1) for i, v in enumerate(sends)]
        homeward = call(
            functools.partial(homeward_body, y_parts),
            [((capacity, part), bf16)] * group,
            (own, *shares),
            name="homeward",
        )
        returned += [swap(v, "sp", first + i) for i, v in enumerate(homeward)]
    (z,) = call(
        functools.partial(combine_body, experts),
        [((tokens, part), bf16)],
        (*returned, ids, pair_weight, normed),
        flops=4 * tokens * experts * capacity * part,
        name="combine",
    )
    (out,) = call(
        norm_body,
        [((tokens, features), bf16)],
        (*over_tp(z, y_parts), out_gain.reshape(1, features)),
        scratch=[pltpu.VMEM((tokens, features), bf16)],
        name="norm",
    )
    return out


def solution(mesh):
    placed = (
        P("sp", "tp"),
        P("sp"),
        P("tp"),
        P("tp", None),
        P("sp", None),
        P(),
        P("sp", None),
        P("sp", None),
        P("sp", None, "tp"),
        P("sp", None, "tp"),
        P("sp", "tp", None),
        P(),
    )
    return jax.shard_map(
        shards, mesh=mesh, in_specs=placed, out_specs=P("sp", None), check_vma=False
    )
```

```python
import functools

import jax
import jax.numpy as jnp
from jax import lax
from jax.experimental import pallas as pl
from jax.experimental.pallas import tpu as pltpu
from jax.sharding import PartitionSpec as P


alpha_res = 1.4142135623730951
norm_eps = 1e-05
reach = 16
lanes = 128
f32, bf16 = jnp.float32, jnp.bfloat16
MIB, GIGA = 2**20, 10**9


def swap(value, axis, bits):
    if bits == 0:
        return value
    count = lax.axis_size(axis)
    return lax.ppermute(value, axis, [(i, i ^ bits) for i in range(count)])


def tiles(total, width):
    return [(at, min(width, total - at)) for at in range(0, total, width)]


def dot(a, b):
    return jnp.dot(a, b, preferred_element_type=f32)


def call(body, outs, operands, scratch=(), flops=3 * GIGA, vmem=16):
    whole = pl.BlockSpec(memory_space=pltpu.VMEM)
    return pl.pallas_call(
        body,
        out_shape=[jax.ShapeDtypeStruct(shape, kind) for shape, kind in outs],
        in_specs=[whole] * len(operands),
        out_specs=[whole] * len(outs),
        scratch_shapes=list(scratch),
        compiler_params=pltpu.CompilerParams(vmem_limit_bytes=vmem * MIB),
        cost_estimate=pl.CostEstimate(flops=flops, bytes_accessed=0, transcendentals=0),
    )(*operands)


def place():
    t = lax.axis_index("tp")
    return t & 1, t >> 1, lax.axis_size("tp") // 2


def columns(start, width):
    return pl.ds(pl.multiple_of(start, lanes), width)


def as_column(row):
    return jnp.broadcast_to(row, (lanes, row.shape[1])).T[:, :1]


def tail_body(x, docs, pack):
    rows = x.shape[0]
    pack[0:reach, :] = x[rows - reach :, :]
    pack[reach:, :] = jnp.zeros((reach, x.shape[1]), bf16)
    pack[reach:, 0:lanes] = jnp.broadcast_to(
        docs[:, rows - lanes :].astype(f32), (reach, lanes)
    ).astype(bf16)


def mix_body(x, pack, docs, scale, weights, keep, send):
    core, _, _ = place()
    rows, cols = x.shape
    half = keep.shape[1]
    window = jnp.left_shift(2, lax.axis_index("tp") * cols // (2 * half // 4))
    doc_row = docs[...].astype(f32)
    doc_col = as_column(doc_row)
    lag = lax.broadcasted_iota(jnp.int32, (rows, rows), 0) - lax.broadcasted_iota(
        jnp.int32, (rows, rows), 1
    )
    band = jnp.where((lag >= 0) & (lag < window) & (doc_col == doc_row), 1.0, 0.0)
    total = dot(band.astype(bf16), x[...])
    count = jnp.sum(band, axis=1, keepdims=True)
    lag_tail = (
        lax.broadcasted_iota(jnp.int32, (reach, lanes), 0)
        + lanes
        - lax.broadcasted_iota(jnp.int32, (reach, lanes), 1)
    )
    tail_doc = pack[reach : reach + 1, 0:lanes].astype(f32)
    inside = (lag_tail < window) & (doc_col[:reach] == tail_doc) & (lax.axis_index("sp") > 0)
    band_tail = jnp.where(inside, 1.0, 0.0)
    before = jnp.concatenate(
        [jnp.zeros((lanes - reach, cols), bf16), pack[0:reach, :]], axis=0
    )
    top = total[:reach] + dot(band_tail.astype(bf16), before)
    top_count = count[:reach] + jnp.sum(band_tail, axis=1, keepdims=True)
    total = jnp.concatenate([top, total[reach:]], axis=0)
    count = jnp.concatenate([top_count, count[reach:]], axis=0)
    mixed = ((total / count - x[...].astype(f32)) * scale[...]).astype(bf16)
    for out, which in ((send, 1 - core), (keep, core)):
        for at, width in tiles(half, 256):
            out[:, at : at + width] = dot(
                mixed, weights[:, columns(which * half + at, width)]
            ).astype(out.dtype)


def split_body(keep, arrived, own, *sends):
    _, y, _ = place()
    part = own.shape[1]
    for bits, out in enumerate((own, *sends)):
        at = columns((y ^ bits) * part, part)
        out[...] = (keep[:, at].astype(f32) + arrived[:, at].astype(f32)).astype(out.dtype)


def stats_body(parts, *refs):
    own, arrived, residual, z_out, stats = refs[0], refs[1:parts], refs[parts], refs[-2], refs[-1]
    width = own.shape[1]
    core, y, y_parts = place()
    z = alpha_res * residual[:, columns((core * y_parts + y) * width, width)].astype(f32)
    shares = own[...]
    for ref in arrived:
        shares = shares + ref[...].astype(f32)
    z = z + shares
    z_out[...] = z
    mean = jnp.mean(z, axis=1, keepdims=True)
    spread = jnp.sum((z - mean) * (z - mean), axis=1, keepdims=True)
    lane = lax.broadcasted_iota(jnp.int32, (z.shape[0], lanes), 1)
    stats[...] = jnp.where(lane == 0, mean, spread).T[0:8, :]


def slot_rows(ids, capacity, experts):
    tokens = ids.shape[1]
    expert = lax.broadcasted_iota(jnp.int32, (experts, tokens), 0)
    first, second = expert == ids[0:1, :], expert == ids[1:2, :]
    named = jnp.where(first | second, 1.0, 0.0)
    earlier = (
        lax.broadcasted_iota(jnp.int32, (tokens, tokens), 0)
        < lax.broadcasted_iota(jnp.int32, (tokens, tokens), 1)
    )
    before = dot(named.astype(bf16), jnp.where(earlier, 1.0, 0.0).astype(bf16))
    slots = []
    for k, mine in enumerate((first, second)):
        rank = jnp.sum(jnp.where(mine, before, 0.0), axis=0, keepdims=True)
        slots.append(ids[k : k + 1, :] * capacity + rank.astype(jnp.int32))
    return slots


def dispatch_body(devices, experts, *refs):
    stats, (z_ref, gain, ids), outs = refs[:devices], refs[devices : devices + 3], refs[devices + 3 :]
    normed_ref, sends = outs[0], outs[1:]
    core, y, y_parts = place()
    tokens, width = z_ref.shape
    capacity = sends[0].shape[0]
    means = [ref[0:1, :] for ref in stats]
    mean = sum(means[1:], means[0]) / devices
    spread = sum(
        (ref[1:2, :] + width * (m - mean) * (m - mean) for ref, m in zip(stats, means)),
        jnp.zeros_like(mean),
    )
    scale = lax.rsqrt(spread / (width * devices) + norm_eps)
    gain_here = gain[:, columns((core * y_parts + y) * width, width)]
    normed = (z_ref[...] - as_column(mean)) * as_column(scale) * gain_here
    normed = normed.astype(bf16)
    normed_ref[...] = normed
    slots = slot_rows(ids, capacity, experts)
    s = lax.axis_index("sp")
    for bits, out in enumerate(sends):
        slot = (s ^ bits) * capacity + lax.broadcasted_iota(jnp.int32, (capacity, tokens), 0)
        chosen = jnp.where((slots[0] == slot) | (slots[1] == slot), 1.0, 0.0)
        out[...] = dot(chosen.astype(bf16), normed).astype(bf16)


def stack_body(*refs):
    out = refs[-1]
    rows = refs[0].shape[0]
    for i, ref in enumerate(refs[:-1]):
        out[i * rows : (i + 1) * rows, :] = ref[...]


def unpack(pieces, wide):
    core, y, y_parts = place()
    width = pieces[0].shape[1]
    for i, ref in enumerate(pieces):
        at = (core ^ (i // y_parts)) * y_parts + (y ^ (i % y_parts))
        wide[:, columns(at * width, width)] = ref[...]


def expert_body(count, *refs):
    pieces, (w_gate, w_up, w_down), (send, keep) = (
        refs[:count],
        refs[count : count + 3],
        refs[count + 3 : count + 5],
    )
    wide, hidden = refs[count + 5 :]
    core, _, _ = place()
    unpack(pieces, wide)
    half = keep.shape[1]
    for at, width in tiles(w_gate.shape[1], 256):
        gate = dot(wide[...], w_gate[:, at : at + width])
        upper = dot(wide[...], w_up[:, at : at + width])
        hidden[:, at : at + width] = (gate / (1.0 + jnp.exp(-gate)) * upper).astype(bf16)
    for out, which in ((send, 1 - core), (keep, core)):
        for at, width in tiles(half, 256):
            out[:, at : at + width] = dot(
                hidden[...], w_down[:, columns(which * half + at, width)]
            ).astype(bf16)


def homeward_body(parts, *refs):
    own, arrived, outs = refs[0], refs[1:parts], refs[parts:]
    rows = outs[0].shape[0]
    total = own[...].astype(f32)
    for ref in arrived:
        total = total + ref[...].astype(f32)
    for i, out in enumerate(outs):
        out[...] = total[i * rows : (i + 1) * rows].astype(bf16)


def combine_body(experts, *refs):
    returned, (ids, pair_weight, normed, z_out) = refs[:experts], refs[experts:]
    capacity = returned[0].shape[0]
    tokens = normed.shape[0]
    slots = slot_rows(ids, capacity, experts)
    s = lax.axis_index("sp")
    z = alpha_res * normed[...].astype(f32)
    for bits, ref in enumerate(returned):
        slot = (s ^ bits) * capacity + lax.broadcasted_iota(jnp.int32, (capacity, tokens), 0)
        chosen = jnp.where(slots[0] == slot, pair_weight[0:1, :], 0.0) + jnp.where(
            slots[1] == slot, pair_weight[1:2, :], 0.0
        )
        high = chosen.astype(bf16)
        low = (chosen - high.astype(f32)).astype(bf16)
        for share in (high, low):
            z = z + lax.dot_general(
                share, ref[...], (((0,), (0,)), ((), ())), preferred_element_type=f32
            )
    z_out[...] = z.astype(bf16)


def norm_body(*refs):
    pieces, gain, out, wide = refs[:-3], refs[-3], refs[-2], refs[-1]
    unpack(pieces, wide)
    z = wide[...].astype(f32)
    centred = z - jnp.mean(z, axis=1, keepdims=True)
    var = jnp.mean(centred * centred, axis=1, keepdims=True)
    out[...] = (centred * lax.rsqrt(var + norm_eps) * gain[...]).astype(bf16)


def over_tp(value, y_parts):
    mine = [swap(value, "tp", i << 1) for i in range(y_parts)]
    return mine + [swap(part, "tp", 1) for part in mine]


chunks = 4


def shards(
    mixer_in,
    doc_ids,
    mix_scale,
    out_proj,
    residual,
    mix_gain,
    expert_ids,
    expert_weight,
    w_gate,
    w_up,
    w_down,
    out_gain,
):
    tokens, cols = mixer_in.shape
    features = mix_gain.shape[0]
    experts, devices = lax.axis_size("sp"), lax.axis_size("tp")
    y_parts = devices // 2
    half, part = features // 2, features // devices
    capacity = 4 * tokens // experts
    ids, pair_weight = expert_ids.T, expert_weight.T

    docs = doc_ids.reshape(1, tokens)
    (pack,) = call(tail_body, [((2 * reach, cols), bf16)], (mixer_in, docs), flops=8 * GIGA)
    pack = lax.ppermute(pack, "sp", [(i, i + 1) for i in range(experts - 1)])
    keep, send = call(
        mix_body,
        [((tokens, half), f32), ((tokens, half), bf16)],
        (mixer_in, pack, docs, mix_scale.reshape(1, cols), out_proj),
        flops=2 * GIGA,
    )
    arrived = swap(send, "tp", 1)
    own, *sends = call(
        split_body,
        [((tokens, part), f32)] + [((tokens, part), bf16)] * (y_parts - 1),
        (keep, arrived),
        flops=10 * GIGA,
    )
    shares = [swap(v, "tp", i << 1) for i, v in enumerate(sends, 1)]
    z, stats = call(
        functools.partial(stats_body, y_parts),
        [((tokens, part), f32), ((8, tokens), f32)],
        (own, *shares, residual),
        flops=6 * GIGA,
    )
    every = [swap(stats, "tp", i) for i in range(devices)]
    normed, *outgoing = call(
        functools.partial(dispatch_body, devices, experts),
        [((tokens, part), bf16)] + [((capacity, part), bf16)] * experts,
        (*every, z, mix_gain.reshape(1, features), ids),
        flops=10 * GIGA,
    )
    incoming = [swap(v, "sp", i) for i, v in enumerate(outgoing)]
    group = experts // chunks
    rows = group * capacity
    returned = []
    for at in range(chunks):
        first = at * group
        (stacked,) = call(stack_body, [((rows, part), bf16)], incoming[first : first + group])
        pieces = over_tp(stacked, y_parts)
        send, keep = call(
            functools.partial(expert_body, len(pieces)),
            [((rows, half), bf16)] * 2,
            (*pieces, w_gate[0], w_up[0], w_down[0]),
            scratch=[
                pltpu.VMEM((rows, features), bf16),
                pltpu.VMEM((rows, w_gate.shape[2]), bf16),
            ],
            flops=6 * rows * features * w_gate.shape[2],
            vmem=16,
        )
        arrived = swap(send, "tp", 1)
        own, *sends = call(split_body, [((rows, part), bf16)] * y_parts, (keep, arrived))
        shares = [swap(v, "tp", i << 1) for i, v in enumerate(sends, 1)]
        homeward = call(
            functools.partial(homeward_body, y_parts),
            [((capacity, part), bf16)] * group,
            (own, *shares),
        )
        returned += [swap(v, "sp", i) for i, v in enumerate(homeward, first)]
    (z,) = call(
        functools.partial(combine_body, experts),
        [((tokens, part), bf16)],
        (*returned, ids, pair_weight, normed),
        flops=4 * tokens * experts * capacity * part,
    )
    (out,) = call(
        norm_body,
        [((tokens, features), bf16)],
        (*over_tp(z, y_parts), out_gain.reshape(1, features)),
        scratch=[pltpu.VMEM((tokens, features), bf16)],
    )
    return out


def solution(mesh):
    placed = (
        P("sp", "tp"),
        P("sp"),
        P("tp"),
        P("tp", None),
        P("sp", None),
        P(),
        P("sp", None),
        P("sp", None),
        P("sp", None, "tp"),
        P("sp", None, "tp"),
        P("sp", "tp", None),
        P(),
    )
    return jax.shard_map(
        shards, mesh=mesh, in_specs=placed, out_specs=P("sp", None), check_vma=False
    )
```
